128 devices in a mesh: kv: 16 (over z, y), tp: 8 (over x, core).
Axes of the slice: x: 4, y: 4, z: 4, core: 2. Of those that a mesh axis runs over, the one named last changes fastest.
Arguments:
- tokens: bfloat16 [64, 4096], P(None, 'kv'), may hold values from -170 to 170
- mix_gain: float32 [4096], P('kv'), may hold values from 0.1 to 1.9
- w_query: bfloat16 [4096, 2048], P('kv', 'tp'), may hold values from -0.09375 to 0.09375
- w_key: bfloat16 [4096, 512], P('kv', 'tp'), may hold values from -0.09375 to 0.09375
- w_value: bfloat16 [4096, 512], P('kv', 'tp'), may hold values from -0.09375 to 0.09375
- w_forget: bfloat16 [4096, 32], P('kv', 'tp'), may hold values from -0.09375 to 0.09375
- query_gain: float32 [64], replicated, may hold values from 0.1 to 1.9
- key_cache: bfloat16 [64, 8, 64, 16384], P(None, 'tp', None, 'kv'), may hold values from -1300 to 1300
- value_cache: bfloat16 [64, 8, 64, 16384], P(None, 'tp', None, 'kv'), may hold values from -8 to 8
- decay_cache: float32 [64, 32, 16384], P(None, 'tp', 'kv'), may hold values from -2131.92 to 0, as said below
- w_out: bfloat16 [2048, 4096], P('tp', 'kv'), may hold values from -1 to 1
- mlp_gain: float32 [4096], P('kv'), may hold values from 0.1 to 1.9
- w_up: bfloat16 [4096, 16384], P('kv', 'tp'), may hold values from -0.09375 to 0.09375
- w_down: bfloat16 [16384, 4096], P('tp', 'kv'), may hold values from -0.046875 to 0.046875
Outputs:
- layer_out: bfloat16 [64, 4096], P(None, 'kv')
The draws below stay inside these ranges and needn't reach their ends.
Inputs may be any that keep to these rules, and one draw needn't show every extreme that they name: `decay_cache`: each entry is the sum of the non-positive log forget gates of the later cached positions of its sequence and head: 0 at the last cached position, never smaller at a later position.
All inputs are finite; a program needn't handle non-finite values.
Results may differ from the reference program's by a relative error of at most 0.015.
Values may be sent and summed in bfloat16 or wider, within the bound.
A program may use at most 64 MiB of HBM per device.

```python
import jax
import jax.numpy as jnp
from jax import lax

D = 4096
HEADS = 32
KV_HEADS = 8
HEAD_DIM = 64
FF = 16384
BATCH = 64
POSITIONS_LOCAL = 1024
POSITIONS = 16384
HEAD_GROUP = 4
FF_GROUP = 2048


def draw_tokens(key, part):
    keys = jax.random.split(key, 2)
    columns = jnp.arange(D, dtype=jnp.float32) / D
    base = jnp.clip(jax.random.normal(keys[0], (BATCH, D), jnp.float32), -4.0, 4.0)
    row_scale = jnp.exp(jax.random.uniform(keys[1], (BATCH, 1), jnp.float32, 0.0, jnp.log(3.0)))
    rising = 3.0 ** columns
    return (base * row_scale * rising[None, :]).astype(jnp.bfloat16)


def draw_key_cache(key, part):
    keys = jax.random.split(key, 3)
    base = jnp.clip(jax.random.normal(keys[0], (BATCH, KV_HEADS, HEAD_DIM, POSITIONS), jnp.float32), -5.0, 5.0)
    low_strength = jnp.log(40.0)
    high_strength = jnp.log(200.0)
    strength = jnp.exp(jax.random.uniform(keys[1], (BATCH, KV_HEADS, 1, 1), jnp.float32, low_strength, high_strength))
    spot = jax.random.randint(keys[2], (BATCH, KV_HEADS, 1, 1), 0, POSITIONS - 1)
    current_location = jnp.arange(POSITIONS).reshape(1, 1, 1, POSITIONS)
    anchor = jnp.take_along_axis(base, jnp.broadcast_to(spot, (BATCH, KV_HEADS, HEAD_DIM, 1)), axis=3)
    bump = jnp.where(current_location == spot + 1, 1.01, 1.0)
    planted = (current_location == spot) | (current_location == spot + 1)
    base = jnp.where(planted, anchor * strength * bump, base)
    return base.astype(jnp.bfloat16)


def draw_value_cache(key, part):
    keys = jax.random.split(key, 2)
    blocks = POSITIONS // POSITIONS_LOCAL
    base = jnp.clip(jax.random.normal(keys[0], (BATCH, KV_HEADS, HEAD_DIM, POSITIONS), jnp.float32), -5.0, 5.0)
    means = jnp.clip(jax.random.normal(keys[1], (BATCH, KV_HEADS, HEAD_DIM, blocks), jnp.float32), -3.0, 3.0)
    return (base + jnp.repeat(means, POSITIONS_LOCAL, axis=3)).astype(jnp.bfloat16)


def draw_decay_cache(key, part):
    keys = jax.random.split(key, 7)
    fast_share = 0.5
    is_fast = jax.random.uniform(keys[0], (BATCH, HEADS, 1), jnp.float32) < fast_share
    slow_rate = jax.random.uniform(keys[1], (BATCH, HEADS, 1), jnp.float32, 0.3, 0.8) / POSITIONS
    fast_rate = jnp.exp(jax.random.uniform(keys[2], (BATCH, HEADS, 1), jnp.float32, jnp.log(0.01), jnp.log(0.04)))
    baseline_rate = jnp.where(is_fast, fast_rate, slow_rate)
    blocks = POSITIONS // POSITIONS_LOCAL
    block_multiplier = jnp.exp(jax.random.uniform(keys[3], (BATCH, HEADS, blocks), jnp.float32, jnp.log(0.5), jnp.log(2.0)))
    coarse_estimate = jax.random.uniform(keys[4], (BATCH, HEADS, POSITIONS), jnp.float32, 0.5, 1.5)
    chosen_places = jax.random.randint(keys[5], (BATCH, HEADS, 2), 0, POSITIONS)
    loss_values = jax.random.uniform(keys[6], (BATCH, HEADS, 2), jnp.float32, 0.22, 0.69)
    current_location = jnp.arange(POSITIONS).reshape(1, 1, POSITIONS)
    sudden_jump = jnp.where(current_location == chosen_places[:, :, 0:1], loss_values[:, :, 0:1], 0.0)
    sudden_jump = sudden_jump + jnp.where(current_location == chosen_places[:, :, 1:2], loss_values[:, :, 1:2], 0.0)
    per_step_rate = baseline_rate * jnp.repeat(block_multiplier, POSITIONS_LOCAL, axis=2) * coarse_estimate + sudden_jump
    after = jnp.flip(jnp.cumsum(jnp.flip(per_step_rate, axis=2), axis=2), axis=2) - per_step_rate
    return -after


def shard_levels(key, extent, cuts, low, high):
    def one(axis_at, blocks):
        draws = jax.random.uniform(jax.random.fold_in(jax.random.fold_in(key, 6), axis_at), (blocks,), jnp.float32, low / len(cuts), high / len(cuts))
        return jnp.repeat(jnp.exp(draws), extent[axis_at] // blocks).reshape((-1,) + (1,) * (len(extent) - axis_at - 1))

    level = one(*cuts[0])
    for cut in cuts[1:]:
        level = level * one(*cut)
    return level


def bell_draw(own_key, dims, scale, limit, shards=(), kind=jnp.bfloat16):
    entries = jax.random.normal(own_key, dims, jnp.float32) * scale
    if len(shards) > 0:
        entries = shard_levels(own_key, dims, shards, -0.22, 0.18) * entries
    return jnp.clip(entries, min=-limit, max=limit).astype(kind)


def setup_inputs(seed: int = 0) -> dict:
    arg_keys = jax.random.split(jax.random.key(seed), 15)
    return {
        "tokens": draw_tokens(jax.random.fold_in(arg_keys[14], 71), 0),
        "mix_gain": jnp.clip(1.0 + 0.18 * jax.random.normal(arg_keys[1], (D,), jnp.float32), 0.1, 1.9),
        "w_query": bell_draw(arg_keys[2], (D, HEADS * HEAD_DIM), D ** -0.5, 0.09375, ((0, 16), (1, 8))),
        "w_key": bell_draw(arg_keys[3], (D, KV_HEADS * HEAD_DIM), D ** -0.5, 0.09375, ((0, 16), (1, 8))),
        "w_value": bell_draw(arg_keys[4], (D, KV_HEADS * HEAD_DIM), D ** -0.5, 0.09375, ((0, 16), (1, 8))),
        "w_forget": bell_draw(arg_keys[5], (D, HEADS), D ** -0.5, 0.09375, ((0, 16), (1, 8))),
        "query_gain": jnp.clip(1.0 + 0.18 * jax.random.normal(arg_keys[6], (HEAD_DIM,), jnp.float32), 0.1, 1.9),
        "key_cache": draw_key_cache(jax.random.fold_in(arg_keys[14], 71), 0),
        "value_cache": draw_value_cache(jax.random.fold_in(arg_keys[14], 71), 0),
        "decay_cache": draw_decay_cache(jax.random.fold_in(arg_keys[14], 71), 0),
        "w_out": bell_draw(arg_keys[10], (HEADS * HEAD_DIM, D), (HEADS * HEAD_DIM // 64) ** -0.5, 1.0, ((0, 8), (1, 16))),
        "mlp_gain": jnp.clip(1.0 + 0.18 * jax.random.normal(arg_keys[11], (D,), jnp.float32), 0.1, 1.9),
        "w_up": bell_draw(arg_keys[12], (D, FF), D ** -0.5, 0.09375, ((0, 16), (1, 8))),
        "w_down": bell_draw(arg_keys[13], (FF, D), FF ** -0.5, 0.046875, ((0, 8), (1, 16))),
    }


EPS = 1e-06

def rounded(value):
    return lax.optimization_barrier(value.astype(jnp.bfloat16)).astype(jnp.float32)

def attend_one(operands):
    query_row, keys_row, values_row, decay_row, forget_row, key_row, value_row = operands
    score_scale = HEAD_DIM ** (-0.5)
    scores = jnp.einsum('gjd,gdp->gjp', query_row.astype(jnp.float32), keys_row.astype(jnp.float32)) * score_scale
    scores = scores + decay_row + forget_row[..., None]
    own_score = jnp.einsum('gjd,gd->gj', query_row.astype(jnp.float32), key_row.astype(jnp.float32)) * score_scale
    peak_score = jnp.maximum(lax.optimization_barrier(jnp.max(scores, axis=-1)), own_score)
    weights = jnp.exp(scores - peak_score[..., None])
    own_weight = jnp.exp(own_score - peak_score)
    totals = lax.optimization_barrier(jnp.sum(weights, axis=-1)) + own_weight
    summed = jnp.einsum('gjp,gdp->gjd', rounded(weights), values_row.astype(jnp.float32))
    summed = summed + rounded(own_weight)[..., None] * value_row.astype(jnp.float32)[:, None, :]
    return summed / totals[..., None]

def reference(tokens, mix_gain, w_query, w_key, w_value, w_forget, query_gain, key_cache, value_cache, decay_cache, w_out, mlp_gain, w_up, w_down):
    stream = tokens.astype(jnp.float32)
    scale_mix = lax.rsqrt(lax.optimization_barrier(jnp.mean(stream * stream, axis=1, keepdims=True)) + EPS)
    normed_mix = (stream * mix_gain.astype(jnp.float32)).astype(jnp.bfloat16)
    query_raw = scale_mix * jnp.dot(normed_mix, w_query, preferred_element_type=jnp.float32)
    key_raw = scale_mix * jnp.dot(normed_mix, w_key, preferred_element_type=jnp.float32)
    value_raw = scale_mix * jnp.dot(normed_mix, w_value, preferred_element_type=jnp.float32)
    forget_raw = scale_mix * jnp.dot(normed_mix, w_forget, preferred_element_type=jnp.float32)
    heads_raw = query_raw.reshape(BATCH, HEADS, HEAD_DIM)
    inverse = lax.rsqrt(lax.optimization_barrier(jnp.mean(heads_raw * heads_raw, axis=-1, keepdims=True)) + EPS)
    query = (heads_raw * inverse * query_gain.astype(jnp.float32)).astype(jnp.bfloat16)
    sharing = HEADS // KV_HEADS
    query = query.reshape(BATCH, KV_HEADS, sharing, HEAD_DIM)
    key_new = key_raw.reshape(BATCH, KV_HEADS, HEAD_DIM).astype(jnp.bfloat16)
    value_new = value_raw.reshape(BATCH, KV_HEADS, HEAD_DIM).astype(jnp.bfloat16)
    log_forget = jax.nn.log_sigmoid(forget_raw).reshape(BATCH, KV_HEADS, sharing)
    decay = decay_cache.reshape(BATCH, KV_HEADS, sharing, -1)
    head_output = lax.map(attend_one, (query, key_cache, value_cache, decay, log_forget, key_new, value_new))
    attended = head_output.reshape(BATCH, HEADS * HEAD_DIM).astype(jnp.bfloat16)
    group_count = HEADS // HEAD_GROUP
    head_width = HEAD_GROUP * HEAD_DIM
    partials = jnp.einsum('bgk,gkd->bgd', attended.reshape(BATCH, group_count, head_width).astype(jnp.float32), w_out.reshape(group_count, head_width, D).astype(jnp.float32))
    attn_out = lax.optimization_barrier(jnp.sum(rounded(partials), axis=1))
    residual = (stream + rounded(attn_out)).astype(jnp.bfloat16)
    residual_wide = residual.astype(jnp.float32)
    scale_mlp = lax.rsqrt(lax.optimization_barrier(jnp.mean(residual_wide * residual_wide, axis=1, keepdims=True)) + EPS)
    normed_mlp = (residual_wide * mlp_gain.astype(jnp.float32)).astype(jnp.bfloat16)
    up_proj = scale_mlp * jnp.dot(normed_mlp, w_up, preferred_element_type=jnp.float32)
    hidden = jnp.square(jax.nn.relu(up_proj)).astype(jnp.bfloat16)
    unit_groups = FF // FF_GROUP
    down_parts = jnp.einsum('bgk,gkd->bgd', hidden.reshape(BATCH, unit_groups, FF_GROUP).astype(jnp.float32), w_down.reshape(unit_groups, FF_GROUP, D).astype(jnp.float32))
    mlp_out = lax.optimization_barrier(jnp.sum(rounded(down_parts), axis=1))
    return (residual_wide + rounded(mlp_out)).astype(jnp.bfloat16)
```

```python
import jax
import jax.numpy as jnp
from jax import lax
from jax.experimental import pallas as pl
from jax.experimental.pallas import tpu as pltpu
from jax.sharding import PartitionSpec as P

D = 4096
HEAD_DIM = 64
EPS = 1e-06
F32 = jnp.float32
BF16 = jnp.bfloat16
FAR_FIRST = (2, 1, 3)
SIDE = 4
ROWS = 64
HALF = 32
GROUPS = 16


def near(d):
    return min(d, SIDE - d)


OFFSETS = sorted(
    [(a, b) for a in range(SIDE) for b in range(SIDE) if a or b],
    key=lambda o: -(near(o[0]) + near(o[1])),
)


def dot(a, b):
    return lax.dot_general(a, b, (((1,), (0,)), ((), ())), preferred_element_type=F32)


def dot_t(a, b):
    return lax.dot_general(a, b, (((1,), (1,)), ((), ())), preferred_element_type=F32)


def three(a):
    top = a.astype(BF16)
    rest = a - top.astype(F32)
    mid = rest.astype(BF16)
    low = (rest - mid.astype(F32)).astype(BF16)
    return top, mid, low


def dot_wide(a, b):
    top, mid, low = three(a)
    return (dot(low, b) + dot(mid, b)) + dot(top, b)


def index(shape, dim):
    return lax.broadcasted_iota(jnp.int32, shape, dim)


def ones_where(cond):
    return jnp.where(cond, 1.0, 0.0).astype(BF16)


def kernel(
    tok_h, mixg_h, wq_h, wk_h, wv_h, wf_h, qg_h, k_h, v_h, d_h, wo_h, mlpg_h, wu_h, wd_h,
    out_ref,
    tok, mixg, wq, wk, wv, wf, qg, kb, vb, db, wo, mlpg, wu, wd,
    load_sem,
    t2, spread, pick, same, e_lse, c_lse, t_key, t_value,
    q_send, q_ra, q_mid, q_rb,
    kv_send, kv_ra, kv_mid, kv_rb,
    t_send, t_ra, t_mid, t_rb,
    qx, ox, lx,
    m_send, m_ra, m_mid, m_rb,
    a_pair, a_pr, a_xs, a_xr, a_full,
    n_send, n_ra, n_mid, n_rb,
    up_send, up_recv, hid,
    b_pair, b_pr, b_xs, b_xr, b_full,
    ar_send_sem, ar_recv_sem,
    tile_send_sem, tile_recv_sem,
    tp_send_sem, tp_recv_sem,
    rs_send_sem, rs_recv_sem, ag_send_sem, ag_recv_sem,
):
    kv = lax.axis_index("kv")
    tp = lax.axis_index("tp")
    z, y = kv // SIDE, kv % SIDE
    x, core = tp // 2, tp % 2
    started = []

    def load(k, src, dst):
        copy = pltpu.make_async_copy(src, dst, load_sem.at[k])
        copy.start()
        return copy

    pairs = (
        (tok_h, tok), (mixg_h, mixg), (wq_h, wq), (wk_h, wk), (wv_h, wv), (wf_h, wf), (qg_h, qg),
        (k_h, kb), (d_h, db), (v_h, vb), (wo_h, wo), (mlpg_h, mlpg), (wu_h, wu), (wd_h, wd),
    )
    loads = [load(k, src, dst) for k, (src, dst) in enumerate(pairs)]

    def at_y(d):
        return {"kv": z * SIDE + (y + d) % SIDE}

    def at_z(d):
        return {"kv": ((z + d) % SIDE) * SIDE + y}

    def at_both(dz, dy):
        return {"kv": ((z + dz) % SIDE) * SIDE + (y + dy) % SIDE}

    def at_x(d):
        return {"tp": ((x + d) % SIDE) * 2 + core}

    partner = {"tp": x * 2 + (1 - core)}

    barrier = pltpu.get_barrier_semaphore()
    for dz, dy in OFFSETS:
        pl.semaphore_signal(barrier, inc=1, device_id=at_both(dz, dy))
    for d in FAR_FIRST:
        pl.semaphore_signal(barrier, inc=1, device_id=at_x(d))
    pl.semaphore_signal(barrier, inc=1, device_id=partner)

    def send(src, dst, send_sem, recv_sem, to):
        copy = pltpu.make_async_remote_copy(
            src_ref=src, dst_ref=dst, send_sem=send_sem, recv_sem=recv_sem, device_id=to
        )
        copy.start()
        started.append(copy)
        return copy

    r, l = index((256, 256), 0), index((256, 256), 1)
    t2[...] = ones_where(r % 64 == l % 64)
    same[...] = ones_where(r // 64 == l // 64)
    r, l = index((256, 64), 0), index((256, 64), 1)
    spread[...] = ones_where(r // 4 == l)
    r, l = index((64, 256), 0), index((64, 256), 1)
    pick[...] = ones_where(l // 4 == r)
    r, l = index((128, 256), 0), index((128, 256), 1)
    e_lse[...] = ones_where((r < 12) & (r % 4 == l // 64))
    t_key[...] = ones_where(r == l % 64)
    t_value[...] = ones_where(r - 64 == l % 64)
    r, l = index((256, 128), 0), index((256, 128), 1)
    for part in range(3):
        c_lse[part] = ones_where((r % 64 == 0) & (l == r // 64 + 4 * part))

    for k in range(6):
        loads[k].wait()
    stream = tok[...].astype(F32)
    normed = (stream * mixg[...]).astype(BF16)
    q_send[...] = dot(normed, wq[...]).astype(BF16)
    diagonal = index((ROWS, ROWS), 0) == index((ROWS, ROWS), 1)

    def to_row(column):
        return jnp.sum(jnp.where(diagonal, column, 0.0), axis=0, keepdims=True)

    def to_column(row):
        return jnp.sum(jnp.where(diagonal, row, 0.0), axis=1, keepdims=True)

    t_send[...] = jnp.zeros_like(t_send)
    t_send[0:4, 0:ROWS] = dot_t(wf[...], normed)
    t_send[4:5, 0:ROWS] = to_row(jnp.sum(stream * stream, axis=1, keepdims=True))
    kv_send[:, 0:64] = dot_t(normed, wk[...]).astype(BF16)
    kv_send[:, 64:128] = dot_t(normed, wv[...]).astype(BF16)

    pl.semaphore_wait(barrier, len(OFFSETS) + 3 + 1)

    def first_leg(block, ra, which):
        copies = []
        for d in FAR_FIRST:
            for half, at in ((0, at_y), (1, at_z)):
                sems = (which, 0, half, d - 1)
                copies.append(
                    (half, send(
                        block.at[pl.ds(half * HALF, HALF)], ra.at[half, d - 1],
                        ar_send_sem.at[sems], ar_recv_sem.at[sems], at(d),
                    ))
                )
        return copies

    def second_leg(mid, rb, half, which):
        copies = []
        for d in FAR_FIRST:
            at = (at_z, at_y)[half]
            sems = (which, 1, half, d - 1)
            copies.append(
                send(
                    mid.at[half], rb.at[half, d - 1],
                    ar_send_sem.at[sems], ar_recv_sem.at[sems], at(d),
                )
            )
        return copies

    def wait_half(copies, half):
        for h, copy in copies:
            if h == half:
                copy.wait_recv()

    def four(own, others):
        a, b, c = (others[d].astype(F32) for d in range(3))
        return (own.astype(F32) + b) + (a + c)

    def sum_first(block, ra, mid, rb, copies, which):
        later = []
        for half in range(2):
            wait_half(copies, half)
            own = block[half * HALF : half * HALF + HALF]
            mid[half] = four(own, [ra[half, d] for d in range(3)]).astype(BF16)
            later.append(second_leg(mid, rb, half, which))
        return later

    def sum_second(mid, rb, later):
        halves = []
        for half in range(2):
            for copy in later[half]:
                copy.wait_recv()
            halves.append(four(mid[half], [rb[half, d] for d in range(3)]))
        return jnp.concatenate(halves, axis=0)

    def tile_leg(src, dst, at, which, leg):
        return [
            send(src, dst.at[d - 1], tile_send_sem.at[which, leg, d - 1],
                 tile_recv_sem.at[which, leg, d - 1], at(d))
            for d in FAR_FIRST
        ]

    def tile_sum(own, others, copies):
        for copy in copies:
            copy.wait_recv()
        return four(own[...], [others[d] for d in range(3)])

    q_first = first_leg(q_send, q_ra, 0)
    t_first = tile_leg(t_send, t_ra, at_y, 0, 0)
    kv_first = first_leg(kv_send, kv_ra, 1)

    q_later = sum_first(q_send, q_ra, q_mid, q_rb, q_first, 0)
    t_mid[...] = tile_sum(t_send, t_ra, t_first)
    t_later = tile_leg(t_mid, t_rb, at_z, 0, 1)
    kv_later = sum_first(kv_send, kv_ra, kv_mid, kv_rb, kv_first, 1)

    loads[6].wait()
    gain = dot_wide(qg[...], t_key[0:64, :])

    query_raw = sum_second(q_mid, q_rb, q_later)
    tile = tile_sum(t_mid, t_rb, t_later)
    scale_mix = lax.rsqrt(to_column(tile[4:5, 0:ROWS]) / D + EPS)
    heads_raw = scale_mix * query_raw
    mean_square = dot_wide(heads_raw * heads_raw, same[...]) / HEAD_DIM
    query = (heads_raw * lax.rsqrt(mean_square + EPS) * gain).astype(BF16)
    r, l = index((256, 256), 0), index((256, 256), 1)
    head_mask = l // 64 == r % 4
    row_mask = l // 64 == (r // 4) % 4
    score_scale = HEAD_DIM ** (-0.5)
    rows = dot(spread[...], query) * score_scale
    rows = jnp.where(head_mask, rows, 0.0).astype(BF16)
    qx[...] = jnp.where(row_mask, dot(rows, t2[...]), 0.0).astype(BF16)

    for k in (7, 8, 9):
        loads[k].wait()

    def attend(g, carry):
        at16 = pl.ds(pl.multiple_of(g * 16, 16), 16)
        at256 = pl.ds(pl.multiple_of(g * 256, 256), 256)
        decay = db[pl.ds(pl.multiple_of(g * 4, 4), 4)].reshape(16, 1024)
        scores = dot(qx[at16, :], kb[at256, :]) + decay
        peak = jnp.max(scores, axis=1, keepdims=True)
        weights = jnp.exp(scores - peak)
        mass = jnp.sum(weights, axis=1, keepdims=True)
        summed = dot_t(weights.astype(BF16), vb[at256, :])
        ox[at16, :] = summed / mass
        lx[at16, :] = jnp.broadcast_to(peak + jnp.log(mass), (16, 128))
        return carry

    lax.fori_loop(0, GROUPS, attend, 0, unroll=4)

    kept = jnp.where(row_mask, ox[...], 0.0).astype(BF16)
    folded = jnp.where(head_mask, dot(kept, t2[...]), 0.0).astype(BF16)
    m_send[:, 0:256] = dot(pick[...], folded).astype(BF16)
    top, mid, low = three(lx[...])
    r, l = index((256, 128), 0), index((256, 128), 1)
    parts = jnp.where(l < 4, top.astype(F32), jnp.where(l < 8, mid.astype(F32), low.astype(F32)))
    parts = jnp.where((l < 12) & (l % 4 == r % 4), parts, 0.0).astype(BF16)
    m_send[:, 256:384] = dot(pick[...], parts).astype(BF16)

    m_first = first_leg(m_send, m_ra, 2)

    kv_sum = (scale_mix * sum_second(kv_mid, kv_rb, kv_later)).astype(BF16)
    key_wide = dot(kv_sum, t_key[...])
    value_wide = dot(kv_sum, t_value[...])
    own_score = dot_wide(query.astype(F32) * key_wide, same[...]) * score_scale
    lane_head = index((ROWS, 256), 1) // 64
    forget = jnp.zeros((ROWS, 256), F32)
    for h in range(4):
        forget = jnp.where(lane_head == h, to_column(tile[h : h + 1, 0:ROWS]), forget)
    log_forget = jax.nn.log_sigmoid(scale_mix * forget)

    def merge(blocks):
        lses = [dot(b[:, 256:384], e_lse[...]) for b in blocks]
        peak = jnp.maximum(jnp.maximum(lses[0], lses[2]), jnp.maximum(lses[1], lses[3]))
        factors = [jnp.exp(v - peak) for v in lses]
        terms = [f * b[:, 0:256].astype(F32) for f, b in zip(factors, blocks)]
        mass = (factors[0] + factors[2]) + (factors[1] + factors[3])
        summed = (terms[0] + terms[2]) + (terms[1] + terms[3])
        return peak, mass, summed

    m_later = []
    for half in range(2):
        wait_half(m_first, half)
        peak, mass, summed = merge(
            [m_send[half * HALF : half * HALF + HALF]] + [m_ra[half, d] for d in range(3)]
        )
        m_mid[half, :, 0:256] = (summed / mass).astype(BF16)
        pieces = three(peak + jnp.log(mass))
        packed = dot(pieces[0], c_lse[0]) + dot(pieces[1], c_lse[1]) + dot(pieces[2], c_lse[2])
        m_mid[half, :, 256:384] = packed.astype(BF16)
        m_later.append(second_leg(m_mid, m_rb, half, 2))

    halves = []
    for half in range(2):
        for copy in m_later[half]:
            copy.wait_recv()
        at = slice(half * HALF, half * HALF + HALF)
        peak, mass, summed = merge([m_mid[half]] + [m_rb[half, d] for d in range(3)])
        far = peak + log_forget[at]
        top = jnp.maximum(far, own_score[at])
        keep = jnp.exp(far - top)
        own_weight = jnp.exp(own_score[at] - top)
        own_rounded = own_weight.astype(BF16).astype(F32)
        totals = mass * keep + own_weight
        halves.append((summed * keep + own_rounded * value_wide[at]) / totals)
    attended = jnp.concatenate(halves, axis=0).astype(BF16)

    def over_tp(terms, pair, pr, xs, xr, full, which):
        pair[...] = terms.astype(BF16).reshape(2, HALF, 256)
        copy = send(pair.at[1 - core], pr, tp_send_sem.at[which, 0], tp_recv_sem.at[which, 0], partner)
        copy.wait_recv()
        xs[...] = (pair[core].astype(F32) + pr[...].astype(F32)).astype(BF16)
        copies = [
            send(xs, xr.at[d - 1], tp_send_sem.at[which, d], tp_recv_sem.at[which, d], at_x(d))
            for d in FAR_FIRST
        ]
        for copy in copies:
            copy.wait_recv()
        return four(xs[...], [xr[d] for d in range(3)])

    def both_halves(value, full, which):
        full[core] = value.astype(BF16)
        copy = send(full.at[core], full.at[core], tp_send_sem.at[which, 4], tp_recv_sem.at[which, 4], partner)
        copy.wait_recv()
        return full[...].reshape(ROWS, 256).astype(F32)

    loads[10].wait()
    attn_half = over_tp(dot(attended, wo[...]), a_pair, a_pr, a_xs, a_xr, a_full, 0)
    attn_out = both_halves(attn_half, a_full, 0)
    residual = (stream + attn_out).astype(BF16)
    residual_wide = residual.astype(F32)
    loads[11].wait()
    loads[12].wait()
    normed_mlp = (residual_wide * mlpg[...]).astype(BF16)
    for j in range(8):
        terms = dot(normed_mlp, wu[:, j * 256 : (j + 1) * 256]).astype(BF16)
        up_send[2 * j] = terms[:, 0:128]
        up_send[2 * j + 1] = terms[:, 128:256]
    rs = []
    for k, (dz, dy) in enumerate(OFFSETS):
        to = at_both(dz, dy)
        rs.append(send(up_send.at[to["kv"]], up_recv.at[k], rs_send_sem.at[k], rs_recv_sem.at[k], to))
    n_send[...] = jnp.zeros_like(n_send)
    n_send[0:1, 0:ROWS] = to_row(jnp.sum(residual_wide * residual_wide, axis=1, keepdims=True))
    n_first = tile_leg(n_send, n_ra, at_y, 1, 0)

    up = up_send[kv].astype(F32)
    for k in reversed(range(len(OFFSETS))):
        rs[k].wait_recv()
        up = up + up_recv[k].astype(F32)
    hid[kv] = jnp.square(jnp.maximum(up, 0.0)).astype(BF16)
    ag = []
    for k, (dz, dy) in enumerate(OFFSETS):
        ag.append(send(hid.at[kv], hid.at[kv], ag_send_sem.at[k], ag_recv_sem.at[k], at_both(dz, dy)))
    n_mid[...] = tile_sum(n_send, n_ra, n_first)
    n_later = tile_leg(n_mid, n_rb, at_z, 1, 1)
    loads[13].wait()
    for k in reversed(range(len(OFFSETS))):
        ag[k].wait_recv()
    down = jnp.zeros((ROWS, 256), F32)
    for j in range(8):
        units = jnp.concatenate([hid[2 * j], hid[2 * j + 1]], axis=1)
        down = down + dot(units, wd[j * 256 : (j + 1) * 256, :])
    down_half = over_tp(down, b_pair, b_pr, b_xs, b_xr, b_full, 1)
    squares = tile_sum(n_mid, n_rb, n_later)
    scale_square = 1.0 / (to_column(squares[0:1, 0:ROWS]) / D + EPS)
    half_scale = jnp.where(core == 0, scale_square[0:HALF], scale_square[HALF:ROWS])
    mlp_out = both_halves(down_half * half_scale, b_full, 1)
    out_ref[...] = (residual_wide + mlp_out).astype(BF16)

    for copy in started:
        copy.wait_send()


def shards(
    tokens, mix_gain, w_query, w_key, w_value, w_forget, query_gain,
    key_cache, value_cache, decay_cache, w_out, mlp_gain, w_up, w_down,
):
    operands = (
        tokens, mix_gain.reshape(1, -1), w_query, w_key.T, w_value.T, w_forget.T,
        query_gain.reshape(1, -1), key_cache.reshape(4096, 1024), value_cache.reshape(4096, 1024),
        decay_cache, w_out, mlp_gain.reshape(1, -1), w_up, w_down,
    )
    vmem = pltpu.VMEM
    dma = pltpu.SemaphoreType.DMA

    def two_legs(width):
        return [
            vmem((ROWS, width), BF16), vmem((2, 3, HALF, width), BF16),
            vmem((2, HALF, width), BF16), vmem((2, 3, HALF, width), BF16),
        ]

    def tile_legs():
        return [vmem((8, 128), F32), vmem((3, 8, 128), F32), vmem((8, 128), F32), vmem((3, 8, 128), F32)]

    def tp_bufs():
        return [
            vmem((2, HALF, 256), BF16), vmem((HALF, 256), BF16), vmem((HALF, 256), BF16),
            vmem((3, HALF, 256), BF16), vmem((2, HALF, 256), BF16),
        ]

    scratch = [vmem(a.shape, a.dtype) for a in operands]
    scratch += [dma((len(operands),))]
    scratch += [
        vmem((256, 256), BF16), vmem((256, 64), BF16), vmem((64, 256), BF16), vmem((256, 256), BF16),
        vmem((128, 256), BF16), vmem((3, 256, 128), BF16), vmem((128, 256), BF16), vmem((128, 256), BF16),
    ]
    scratch += two_legs(256) + two_legs(128) + tile_legs()
    scratch += [vmem((256, 256), BF16), vmem((256, 256), F32), vmem((256, 128), F32)]
    scratch += two_legs(384) + tp_bufs() + tile_legs()
    scratch += [vmem((16, ROWS, 128), BF16), vmem((15, ROWS, 128), BF16), vmem((16, ROWS, 128), BF16)]
    scratch += tp_bufs()
    scratch += [dma((3, 2, 2, 3)), dma((3, 2, 2, 3)), dma((2, 2, 3)), dma((2, 2, 3)), dma((2, 5)), dma((2, 5))]
    scratch += [dma((15,))] * 4
    return pl.pallas_call(
        kernel,
        out_shape=jax.ShapeDtypeStruct((ROWS, 256), BF16),
        in_specs=[pl.BlockSpec(memory_space=pl.ANY)] * len(operands),
        out_specs=pl.BlockSpec(memory_space=pltpu.VMEM),
        scratch_shapes=scratch,
        compiler_params=pltpu.CompilerParams(
            collective_id=0, has_side_effects=True, vmem_limit_bytes=60 * 2**20
        ),
    )(*operands)


def solution(mesh):
    return jax.shard_map(
        shards,
        mesh=mesh,
        in_specs=(
            P(None, "kv"),
            P("kv"),
            P("kv", "tp"),
            P("kv", "tp"),
            P("kv", "tp"),
            P("kv", "tp"),
            P(),
            P(None, "tp", None, "kv"),
            P(None, "tp", None, "kv"),
            P(None, "tp", "kv"),
            P("tp", "kv"),
            P("kv"),
            P("kv", "tp"),
            P("tp", "kv"),
        ),
        out_specs=P(None, "kv"),
        check_vma=False,
    )
```
